32 devices in a mesh: sp: 8 (over z, y), tp: 4 (over x, core).
Axes of the slice: x: 2, y: 2, z: 4, core: 2. Of those that a mesh axis runs over, the one named last changes fastest.
Arguments:
- queries: bfloat16 [8192, 512], P('sp', 'tp'), may hold values from -6 to 6
- keys: bfloat16 [8192, 512], P('sp', 'tp'), may hold values from -6 to 6
- values: bfloat16 [8192, 1024], P('sp', 'tp'), may hold values from -6 to 6
- out_gate: bfloat16 [8192, 1024], P('sp', 'tp'), may hold values from -6 to 6
- decay_logit: float32 [2, 8192, 512], P(None, 'sp', 'tp'), may hold values from -8 to 16
- head_gain: float32 [1024], P('tp'), may hold values from 0.1 to 1.9
- out_weight: bfloat16 [1024, 2048], replicated, may hold values from -0.1875 to 0.1875
- stream: bfloat16 [8192, 2048], P(('sp', 'tp')), may hold values from -6 to 6
- mlp_gain: float32 [2048], replicated, may hold values from 0.1 to 1.9
- up_weight: bfloat16 [2048, 8192], P('sp', 'tp'), may hold values from -0.125 to 0.125
- down_weight: bfloat16 [8192, 2048], P('tp', 'sp'), may hold values from -0.0625 to 0.0625
Outputs:
- output: bfloat16 [8192, 2048], P(('sp', 'tp'))
The draws below stay inside these ranges and needn't reach their ends.
All inputs are finite; a program needn't handle non-finite values.
Results may differ from the reference program's by a relative error of at most 0.018.
Values may be sent and summed in bfloat16 or wider, within the bound.
A program may use at most 128 MiB of HBM per device.

```python
import math
import jax
import jax.numpy as jnp
from jax import lax

D = 2048
HEADS = 8
HEAD_K = 64
HEAD_V = 128
FF = 8192
BLOCK = 64
TOK_DEV = 1024
SEQUENCE_TOKENS = 8192
KEY_W = 512
VALUE_W = 1024
N_TP = 4


def draw_decay_logit(key, part):
    partition_key = jax.random.split(key, 6)
    number_of_heads = KEY_W // HEAD_K
    shard_count = SEQUENCE_TOKENS // TOK_DEV
    fast_share = 0.5
    noise = 0.6 * jax.random.truncated_normal(partition_key[2], -3.0, 3.0, (2, SEQUENCE_TOKENS, number_of_heads, HEAD_K), jnp.float32)
    fast_heads = jax.random.bernoulli(partition_key[0], fast_share, (2, 1, number_of_heads, 1))
    shard_shift = jnp.repeat(jax.random.uniform(partition_key[1], (2, shard_count, 1, 1), jnp.float32, -0.7, 0.7), TOK_DEV, axis=1)
    channel_shift = jax.random.uniform(partition_key[3], (2, 1, number_of_heads, HEAD_K), jnp.float32, -1.0, 1.0)
    slow_level = math.log(SEQUENCE_TOKENS / 16.0) + 2.0 + shard_shift + channel_shift + noise
    fast_level = 1.0 + shard_shift + 0.5 * channel_shift + noise
    magnitude = jnp.where(fast_heads, fast_level, slow_level)
    spike_position = jax.random.randint(partition_key[4], (2, 4, 1), 0, SEQUENCE_TOKENS)
    token_positions = jnp.arange(SEQUENCE_TOKENS, dtype=jnp.int32)[None, None, :]
    spike_row_list = jnp.any(token_positions == spike_position, axis=1)
    spike_magnitude = jax.random.uniform(partition_key[5], (2, SEQUENCE_TOKENS, number_of_heads, 1), jnp.float32, -8.0, -4.0)
    magnitude = jnp.where(spike_row_list[:, :, None, None], spike_magnitude, magnitude)
    return magnitude.reshape(2, SEQUENCE_TOKENS, KEY_W).astype(jnp.float32)


def block_levels(key, shape, cuts, least, top_value):
    loudness = 1.0
    for axis_at, shards_of in cuts:
        heights = jax.random.uniform(jax.random.fold_in(jax.random.fold_in(key, 6), axis_at), (shards_of,), jnp.float32, least / len(cuts), top_value / len(cuts))
        loudness = loudness * jnp.repeat(jnp.exp(heights), shape[axis_at] // shards_of).reshape((-1,) + (1,) * (len(shape) - 1 - axis_at))
    return loudness


def normal_values(key, shape, width, bound, cuts=(), kind=jnp.bfloat16):
    gain = block_levels(key, shape, cuts, -0.22, 0.18) if cuts else 1.0
    result = jax.random.normal(key, shape, jnp.float32) * width * gain
    return jnp.minimum(jnp.maximum(result, -bound), bound).astype(kind)


def setup_inputs(seed: int = 0) -> dict:
    streams_of = jax.random.split(jax.random.key(seed), 12)
    queries = normal_values(streams_of[0], (SEQUENCE_TOKENS, KEY_W), 1.0, 6.0, ((0, 8), (1, 4)))
    keys = normal_values(streams_of[1], (SEQUENCE_TOKENS, KEY_W), 1.0, 6.0, ((0, 8), (1, 4)))
    values = normal_values(streams_of[2], (SEQUENCE_TOKENS, VALUE_W), 1.0, 6.0, ((0, 8), (1, 4)))
    out_gate = normal_values(streams_of[3], (SEQUENCE_TOKENS, VALUE_W), 1.0, 6.0, ((0, 8), (1, 4)))
    decay_logit = draw_decay_logit(jax.random.fold_in(streams_of[11], 71), 0)
    head_gain = jnp.clip(1.0 + 0.18 * jax.random.normal(streams_of[5], (VALUE_W,), jnp.float32), 0.1, 1.9)
    out_weight = normal_values(streams_of[6], (VALUE_W, D), VALUE_W ** -0.5, 0.1875)
    stream = normal_values(streams_of[7], (SEQUENCE_TOKENS, D), 1.0, 6.0, ((0, 32),))
    mlp_gain = jnp.clip(1.0 + 0.18 * jax.random.normal(streams_of[8], (D,), jnp.float32), 0.1, 1.9)
    up_weight = normal_values(streams_of[9], (D, FF), D ** -0.5, 0.125, ((0, 8), (1, 4)))
    down_weight = normal_values(streams_of[10], (FF, D), FF ** -0.5, 0.0625, ((0, 4), (1, 8)))
    return dict(queries=queries, keys=keys, values=values, out_gate=out_gate, decay_logit=decay_logit, head_gain=head_gain, out_weight=out_weight, stream=stream, mlp_gain=mlp_gain, up_weight=up_weight, down_weight=down_weight)


gate_temper = 16.0
norm_eps = 1e-06
highest = lax.Precision.HIGHEST

def blockwise(query_rows, key_rows, value_rows, log_decay):
    length, number_of_heads, key_size = query_rows.shape
    value_size = value_rows.shape[2]
    block_count = length // BLOCK
    query_blk = query_rows.reshape(block_count, BLOCK, number_of_heads, key_size)
    key_blk = key_rows.reshape(block_count, BLOCK, number_of_heads, key_size)
    value_blk = value_rows.reshape(block_count, BLOCK, number_of_heads, value_size)
    within = jnp.cumsum(log_decay.reshape(block_count, BLOCK, number_of_heads, key_size), axis=1)
    block_end = within[:, -1]
    query_dec = query_blk * jnp.exp(within)
    key_inv = key_blk * jnp.exp(-within)
    key_end = key_blk * jnp.exp(block_end[:, None] - within)
    lower_mask = jnp.tril(jnp.ones((BLOCK, BLOCK), dtype=bool))
    scores = jnp.einsum('nihd,njhd->nhij', query_dec, key_inv, precision=highest)
    scores = jnp.where(lower_mask, scores, jnp.float32(0.0))
    intra_out = jnp.einsum('nhij,njhe->nihe', scores, value_blk, precision=highest)
    increments = jnp.einsum('njhd,njhe->nhde', key_end, value_blk, precision=highest)

    def advance(carried, inputs):
        decay_end, increment = inputs
        return (decay_end[..., None] * carried + increment, carried)
    start_state = jnp.zeros((number_of_heads, key_size, value_size), jnp.float32)
    state_end, state_in = lax.scan(advance, start_state, (jnp.exp(block_end), increments))
    inter_out = jnp.einsum('nihd,nhde->nihe', query_dec, state_in, precision=highest)
    return ((intra_out + inter_out).reshape(length, number_of_heads, value_size), state_end)

def reference(queries, keys, values, out_gate, decay_logit, head_gain, out_weight, stream, mlp_gain, up_weight, down_weight):
    length = queries.shape[0]
    query_heads = queries.astype(jnp.float32).reshape(length, HEADS, HEAD_K) * HEAD_K ** (-0.5)
    key_heads = keys.astype(jnp.float32).reshape(length, HEADS, HEAD_K)
    value_heads = values.astype(jnp.float32).reshape(length, HEADS, HEAD_V)
    log_decay = (jax.nn.log_sigmoid(decay_logit) / gate_temper).reshape(2, length, HEADS, HEAD_K)
    forward_out = blockwise(query_heads, key_heads, value_heads, log_decay[0])[0]
    backward_out = blockwise(jnp.flip(query_heads, 0), jnp.flip(key_heads, 0), jnp.flip(value_heads, 0), jnp.flip(log_decay[1], 0))[0]
    attended = forward_out + jnp.flip(backward_out, 0)
    inv_rms = lax.rsqrt(lax.optimization_barrier(jnp.mean(attended * attended, axis=-1, keepdims=True)) + norm_eps)
    normed_heads = (attended * inv_rms * head_gain.reshape(HEADS, HEAD_V)).reshape(length, VALUE_W)
    gated = (normed_heads * jax.nn.silu(out_gate.astype(jnp.float32))).astype(jnp.bfloat16)
    residual = (stream.astype(jnp.float32) + jnp.dot(gated, out_weight, preferred_element_type=jnp.float32)).astype(jnp.bfloat16)
    group_width = FF // N_TP

    def feed_forward(block_rows):
        widened = block_rows.astype(jnp.float32)
        row_rms = lax.rsqrt(lax.optimization_barrier(jnp.mean(widened * widened, axis=-1, keepdims=True)) + norm_eps)
        normed = (widened * row_rms * mlp_gain).astype(jnp.bfloat16)
        hidden = jnp.square(jax.nn.relu(jnp.dot(normed, up_weight, preferred_element_type=jnp.float32))).astype(jnp.bfloat16)
        summed = jnp.zeros(widened.shape, jnp.float32)
        for group in range(N_TP):
            group_part = jnp.dot(hidden[:, group * group_width:(group + 1) * group_width], down_weight[group * group_width:(group + 1) * group_width], preferred_element_type=jnp.float32).astype(jnp.bfloat16)
            group_part = lax.optimization_barrier(group_part)
            summed = summed + group_part.astype(jnp.float32)
        return (widened + summed).astype(jnp.bfloat16)
    output = lax.map(feed_forward, residual.reshape(length // TOK_DEV, TOK_DEV, D))
    return output.reshape(length, D)
```

```python
import functools
import jax
import jax.numpy as jnp
from jax import lax
from jax.experimental import pallas as pl
from jax.experimental.pallas import tpu as pltpu
from jax.sharding import PartitionSpec as P

HEAD_K = 64
HEAD_V = 128
CHUNK = 128
gate_temper = 16.0
norm_eps = 1e-06
MESH = pl.DeviceIdType.MESH
f32 = jnp.float32
bf16 = jnp.bfloat16


def dot(a, b):
    return jnp.dot(a, b, preferred_element_type=f32)


def dot_t0(a, b):
    return lax.dot_general(a, b, (((0,), (0,)), ((), ())), preferred_element_type=f32)


def dot_t1(a, b):
    return lax.dot_general(a, b, (((1,), (1,)), ((), ())), preferred_element_type=f32)


def split_hi_lo(x):
    hi = x.astype(bf16)
    return hi, (x - hi.astype(f32)).astype(bf16)


def attention_kernel(
    sp, tp,
    q_ref, k_ref, v_ref, gate_ref, decay_ref, gain_ref, stream_ref,
    stream_all, gated_all,
    q_dec, out_acc, inc, dec, state_in, msg, got, gbuf,
    st_send, st_recv, sx_send, sx_recv, gx_send, gx_recv, loc_sem,
):
    me_sp, me_tp = lax.axis_index("sp"), lax.axis_index("tp")
    rows, key_w = q_ref.shape
    chunks = rows // CHUNK
    heads = key_w // HEAD_K
    own_rows = stream_ref.shape[0]
    val_w = v_ref.shape[1]

    barrier = pltpu.get_barrier_semaphore()
    for o in range(1, sp):
        pl.semaphore_signal(barrier, inc=1, device_id=(lax.rem(me_sp + o, sp), me_tp), device_id_type=MESH)
    for o in range(1, tp):
        pl.semaphore_signal(barrier, inc=1, device_id=(me_sp, lax.rem(me_tp + o, tp)), device_id_type=MESH)
    pl.semaphore_wait(barrier, sp + tp - 2)

    own_span = pl.ds(pl.multiple_of(me_tp * own_rows, own_rows), own_rows)
    stream_copies = []
    for o in range(1, tp):
        copy = pltpu.make_async_remote_copy(
            src_ref=stream_ref, dst_ref=stream_all.at[own_span, :],
            send_sem=sx_send.at[o - 1], recv_sem=sx_recv.at[o - 1],
            device_id=(me_sp, lax.rem(me_tp + o, tp)), device_id_type=MESH,
        )
        copy.start()
        stream_copies.append(copy)
    own_stream = pltpu.make_async_copy(stream_ref, stream_all.at[own_span, :], loc_sem.at[0])
    own_stream.start()

    row = lax.broadcasted_iota(jnp.int32, (CHUNK, CHUNK), 0)
    col = lax.broadcasted_iota(jnp.int32, (CHUNK, CHUNK), 1)
    lower = row >= col
    upper = row <= col
    tri = (lower.astype(f32).astype(bf16), upper.astype(f32).astype(bf16))
    ones = jnp.ones((2 * CHUNK, HEAD_V), bf16)
    lane = lax.broadcasted_iota(jnp.int32, (CHUNK, key_w), 1)
    head_mask = [(lane >= h * HEAD_K) & (lane < (h + 1) * HEAD_K) for h in range(heads)]
    zero = jnp.zeros((CHUNK, key_w), bf16)

    def first(c, carry):
        span = pl.ds(pl.multiple_of(c * CHUNK, CHUNK), CHUNK)
        q = q_ref[span, :].astype(f32) * HEAD_K ** (-0.5)
        k = k_ref[span, :].astype(f32)
        v = v_ref[span, :]
        scores = [None, None]
        for way in range(2):
            x = decay_ref[way, span, :]
            logd = (jnp.minimum(x, 0.0) - jnp.log1p(jnp.exp(-jnp.abs(x)))) * (1.0 / gate_temper)
            hi, lo = split_hi_lo(logd)
            within = dot(tri[way], hi) + dot(tri[way], lo)
            end = within[CHUNK - 1 : CHUNK, :] if way == 0 else within[0:1, :]
            qd = (q * jnp.exp(within)).astype(bf16)
            ki = (k * jnp.exp(-within)).astype(bf16)
            ke = (k * jnp.exp(end - within)).astype(bf16)
            q_dec[way, span, :] = qd
            scores[way] = [dot_t1(jnp.where(m, qd, zero), ki) for m in head_mask]
            full = dot_t0(ke, v)
            inc[way, c] = jnp.concatenate(
                [full[h * HEAD_K : (h + 1) * HEAD_K, h * HEAD_V : (h + 1) * HEAD_V] for h in range(heads)], axis=0
            )
            dec[way, c] = jnp.exp(dot_t0(jnp.concatenate([hi, lo], axis=0), ones))
        for h in range(heads):
            s = jnp.where(lower, scores[0][h], 0.0) + jnp.where(upper, scores[1][h], 0.0)
            out_acc[span, h * HEAD_V : (h + 1) * HEAD_V] = dot(s.astype(bf16), v[:, h * HEAD_V : (h + 1) * HEAD_V])
        return carry

    lax.fori_loop(0, chunks, first, 0)

    state_shape = (key_w, HEAD_V)
    for way in range(2):

        def total(i, carry):
            state, decay = carry
            c = i if way == 0 else chunks - 1 - i
            d = dec[way, c]
            return d * state + inc[way, c], d * decay

        state, decay = lax.fori_loop(0, chunks, total, (jnp.zeros(state_shape, f32), jnp.ones(state_shape, f32)))
        msg[way, 0:key_w, :] = state.astype(bf16)
        msg[way, key_w : 2 * key_w, :] = decay.astype(bf16)

    got[me_sp] = jnp.zeros(got.shape[1:], bf16)
    state_copies = []
    for o in range(1, sp):
        peer = lax.rem(me_sp + o, sp)
        way = jnp.where(peer > me_sp, 0, 1)
        copy = pltpu.make_async_remote_copy(
            src_ref=msg.at[way], dst_ref=got.at[me_sp],
            send_sem=st_send.at[o - 1], recv_sem=st_recv.at[o - 1],
            device_id=(peer, me_tp), device_id_type=MESH,
        )
        copy.start()
        state_copies.append(copy)
    for copy in state_copies:
        copy.wait()

    for way in range(2):

        def hop(i, state):
            at = i if way == 0 else sp - 1 - i
            reached = at < me_sp if way == 0 else at > me_sp
            block = got[at]
            new = block[key_w : 2 * key_w, :].astype(f32) * state + block[0:key_w, :].astype(f32)
            return jnp.where(reached, new, state)

        start = lax.fori_loop(0, sp, hop, jnp.zeros(state_shape, f32))

        def enter(i, state):
            c = i if way == 0 else chunks - 1 - i
            state_in[c, way * key_w : (way + 1) * key_w, :] = state.astype(bf16)
            return dec[way, c] * state + inc[way, c]

        lax.fori_loop(0, chunks, enter, start)

    def second(c, carry):
        span = pl.ds(pl.multiple_of(c * CHUNK, CHUNK), CHUNK)
        qf, qb = q_dec[0, span, :], q_dec[1, span, :]
        state = state_in[c]
        for h in range(heads):
            cols = slice(h * HEAD_V, (h + 1) * HEAD_V)
            m = head_mask[h]
            both = jnp.concatenate([jnp.where(m, qf, zero), jnp.where(m, qb, zero)], axis=1)
            att = out_acc[span, cols] + dot(both, state)
            inv = lax.rsqrt(jnp.mean(att * att, axis=-1, keepdims=True) + norm_eps)
            g = gate_ref[span, cols].astype(f32)
            silu = g / (1.0 + jnp.exp(-g))
            gbuf[span, cols] = (att * inv * gain_ref[0:1, cols] * silu).astype(bf16)
        return carry

    own_cols = pl.ds(pl.multiple_of(me_tp * val_w, val_w), val_w)
    gated_copies = []
    half = chunks // 2
    for part in range(2):
        lax.fori_loop(part * half, (part + 1) * half, second, 0)
        span = pl.ds(part * half * CHUNK, half * CHUNK)
        for o in range(1, tp):
            copy = pltpu.make_async_remote_copy(
                src_ref=gbuf.at[span, :], dst_ref=gated_all.at[span, own_cols],
                send_sem=gx_send.at[part, o - 1], recv_sem=gx_recv.at[part, o - 1],
                device_id=(me_sp, lax.rem(me_tp + o, tp)), device_id_type=MESH,
            )
            copy.start()
            gated_copies.append(copy)
    own_gated = pltpu.make_async_copy(gbuf, gated_all.at[:, own_cols], loc_sem.at[1])
    own_gated.start()
    for copy in stream_copies + gated_copies:
        copy.wait()
    own_stream.wait()
    own_gated.wait()


def attention(queries, keys, values, out_gate, decay_logit, head_gain, stream):
    sp, tp = lax.axis_size("sp"), lax.axis_size("tp")
    rows, key_w = queries.shape
    val_w = values.shape[1]
    chunks = rows // CHUNK
    own_rows, width = stream.shape
    vmem = pl.BlockSpec(memory_space=pltpu.VMEM)
    hbm = pl.BlockSpec(memory_space=pl.ANY)
    dma = pltpu.SemaphoreType.DMA
    return pl.pallas_call(
        functools.partial(attention_kernel, sp, tp),
        out_shape=(
            jax.ShapeDtypeStruct((own_rows * tp, width), bf16),
            jax.ShapeDtypeStruct((rows, val_w * tp), bf16),
        ),
        in_specs=[vmem] * 7,
        out_specs=(hbm, hbm),
        scratch_shapes=[
            pltpu.VMEM((2, rows, key_w), bf16),
            pltpu.VMEM((rows, val_w), f32),
            pltpu.VMEM((2, chunks, key_w, HEAD_V), f32),
            pltpu.VMEM((2, chunks, key_w, HEAD_V), f32),
            pltpu.VMEM((chunks, 2 * key_w, HEAD_V), bf16),
            pltpu.VMEM((2, 2 * key_w, HEAD_V), bf16),
            pltpu.VMEM((sp, 2 * key_w, HEAD_V), bf16),
            pltpu.VMEM((rows, val_w), bf16),
            dma((sp - 1,)), dma((sp - 1,)), dma((tp - 1,)), dma((tp - 1,)),
            dma((2, tp - 1)), dma((2, tp - 1)), dma((2,)),
        ],
        cost_estimate=pl.CostEstimate(flops=40_000_000_000, bytes_accessed=50_000_000, transcendentals=0),
        compiler_params=pltpu.CompilerParams(collective_id=0, has_side_effects=True),
        name="attention",
    )(queries, keys, values, out_gate, decay_logit, head_gain.reshape(1, val_w), stream)


def local(
    queries, keys, values, out_gate, decay_logit, head_gain, out_weight, stream, mlp_gain, up_weight, down_weight
):
    up_full = lax.all_gather(up_weight, "sp", axis=0, tiled=True)
    sp = lax.axis_size("sp")
    tp_index = lax.axis_index("tp")
    part_w = down_weight.shape[1] // 2
    down_parts = [
        lax.all_gather(down_weight[:, i * part_w : (i + 1) * part_w], "sp", axis=1, tiled=True) for i in range(2)
    ]
    stream_all, gated_all = attention(queries, keys, values, out_gate, decay_logit, head_gain, stream)
    own_rows = stream.shape[0]
    residual = (
        jnp.dot(gated_all, out_weight, preferred_element_type=f32) + stream_all.astype(f32)
    ).astype(bf16)
    wide = residual.astype(f32)
    normed = (wide * lax.rsqrt(jnp.mean(wide * wide, axis=-1, keepdims=True) + norm_eps) * mlp_gain).astype(bf16)
    hidden = jnp.square(jax.nn.relu(jnp.dot(normed, up_full, preferred_element_type=f32))).astype(bf16)
    hidden = lax.optimization_barrier(hidden)
    sums = [
        lax.psum_scatter(
            jnp.dot(hidden, part, preferred_element_type=f32).astype(bf16), "tp", scatter_dimension=0, tiled=True
        ).reshape(own_rows, sp, part_w)
        for part in down_parts
    ]
    mlp_sum = jnp.concatenate(sums, axis=2).reshape(own_rows, sp * 2 * part_w).astype(f32)
    own = lax.dynamic_slice_in_dim(residual, tp_index * own_rows, own_rows, 0)
    return (own.astype(f32) + mlp_sum).astype(bf16)


def solution(mesh):
    in_specs = (
        P("sp", "tp"), P("sp", "tp"), P("sp", "tp"), P("sp", "tp"), P(None, "sp", "tp"), P("tp"), P(),
        P(("sp", "tp"), None), P(), P("sp", "tp"), P("tp", "sp"),
    )
    return jax.shard_map(local, mesh=mesh, in_specs=in_specs, out_specs=P(("sp", "tp"), None), check_vma=False)
```

```python
import functools
import jax
import jax.numpy as jnp
from jax import lax
from jax.experimental import pallas as pl
from jax.experimental.pallas import tpu as pltpu
from jax.sharding import PartitionSpec as P

HEAD_K = 64
HEAD_V = 128
CHUNK = 128
gate_temper = 16.0
norm_eps = 1e-06
MESH = pl.DeviceIdType.MESH
f32 = jnp.float32
bf16 = jnp.bfloat16


def dot(a, b):
    return jnp.dot(a, b, preferred_element_type=f32)


def dot_t0(a, b):
    return lax.dot_general(a, b, (((0,), (0,)), ((), ())), preferred_element_type=f32)


def dot_t1(a, b):
    return lax.dot_general(a, b, (((1,), (1,)), ((), ())), preferred_element_type=f32)


def split_hi_lo(x):
    hi = x.astype(bf16)
    return hi, (x - hi.astype(f32)).astype(bf16)


def attention_kernel(
    sp, tp,
    q_ref, k_ref, v_ref, gate_ref, decay_ref, gain_ref, stream_ref, down_ref,
    stream_all, gated_all, down_all,
    q_dec, out_acc, inc, dec, state_in, msg, got, gbuf,
    st_send, st_recv, sx_send, sx_recv, gx_send, gx_recv, dn_send, dn_recv, loc_sem,
):
    me_sp, me_tp = lax.axis_index("sp"), lax.axis_index("tp")
    rows, key_w = q_ref.shape
    chunks = rows // CHUNK
    heads = key_w // HEAD_K
    own_rows = stream_ref.shape[0]
    val_w = v_ref.shape[1]

    barrier = pltpu.get_barrier_semaphore()
    for o in range(1, sp):
        pl.semaphore_signal(barrier, inc=1, device_id=(lax.rem(me_sp + o, sp), me_tp), device_id_type=MESH)
    for o in range(1, tp):
        pl.semaphore_signal(barrier, inc=1, device_id=(me_sp, lax.rem(me_tp + o, tp)), device_id_type=MESH)
    pl.semaphore_wait(barrier, sp + tp - 2)

    depth, part_w = down_ref.shape
    steps = sp // 2

    def ring_place(i):
        return jnp.where(lax.rem(i, 2) == 0, i // 2, sp - 1 - i // 2)

    def ring_device(p):
        return jnp.where(p < steps, 2 * p, 2 * (sp - 1 - p) + 1)

    place = ring_place(me_sp)

    def ring_copies(step):
        made = []
        for way in range(2):
            sign = 1 if way == 0 else -1
            owner = ring_device(lax.rem(place - sign * (step - 1) + sp, sp))
            peer = ring_device(lax.rem(place + sign + sp, sp))
            span = pl.ds(way * (depth // 2), depth // 2) if step == steps else pl.ds(0, depth)
            cols = pl.ds(pl.multiple_of(owner * part_w, part_w), part_w)
            src = down_ref.at[span, :] if step == 1 else down_all.at[span, cols]
            made.append(pltpu.make_async_remote_copy(
                src_ref=src, dst_ref=down_all.at[span, cols],
                send_sem=dn_send.at[way, step - 1], recv_sem=dn_recv.at[way, step - 1],
                device_id=(peer, me_tp), device_id_type=MESH,
            ))
        return made

    ring = [ring_copies(step) for step in range(1, steps + 1)]

    def ring_start(step):
        for way in range(2):
            if step > 1:
                ring[step - 2][way].wait_recv()
            ring[step - 1][way].start()

    ring_start(1)
    own_down = pltpu.make_async_copy(
        down_ref, down_all.at[:, pl.ds(pl.multiple_of(me_sp * part_w, part_w), part_w)], loc_sem.at[2]
    )
    own_down.start()
    own_span = pl.ds(pl.multiple_of(me_tp * own_rows, own_rows), own_rows)
    stream_copies = []
    for o in range(1, tp):
        copy = pltpu.make_async_remote_copy(
            src_ref=stream_ref, dst_ref=stream_all.at[own_span, :],
            send_sem=sx_send.at[o - 1], recv_sem=sx_recv.at[o - 1],
            device_id=(me_sp, lax.rem(me_tp + o, tp)), device_id_type=MESH,
        )
        copy.start()
        stream_copies.append(copy)
    own_stream = pltpu.make_async_copy(stream_ref, stream_all.at[own_span, :], loc_sem.at[0])
    own_stream.start()

    row = lax.broadcasted_iota(jnp.int32, (CHUNK, CHUNK), 0)
    col = lax.broadcasted_iota(jnp.int32, (CHUNK, CHUNK), 1)
    lower = row >= col
    upper = row <= col
    tri = (lower.astype(f32).astype(bf16), upper.astype(f32).astype(bf16))
    ones = jnp.ones((2 * CHUNK, HEAD_V), bf16)
    lane = lax.broadcasted_iota(jnp.int32, (CHUNK, key_w), 1)
    head_mask = [(lane >= h * HEAD_K) & (lane < (h + 1) * HEAD_K) for h in range(heads)]
    zero = jnp.zeros((CHUNK, key_w), bf16)

    def first(c, carry):
        span = pl.ds(pl.multiple_of(c * CHUNK, CHUNK), CHUNK)
        q = q_ref[span, :].astype(f32) * HEAD_K ** (-0.5)
        k = k_ref[span, :].astype(f32)
        v = v_ref[span, :]
        scores = [None, None]
        for way in range(2):
            x = decay_ref[way, span, :]
            logd = (jnp.minimum(x, 0.0) - jnp.log1p(jnp.exp(-jnp.abs(x)))) * (1.0 / gate_temper)
            hi, lo = split_hi_lo(logd)
            within = dot(tri[way], hi) + dot(tri[way], lo)
            end = within[CHUNK - 1 : CHUNK, :] if way == 0 else within[0:1, :]
            qd = (q * jnp.exp(within)).astype(bf16)
            ki = (k * jnp.exp(-within)).astype(bf16)
            ke = (k * jnp.exp(end - within)).astype(bf16)
            q_dec[way, span, :] = qd
            scores[way] = [dot_t1(jnp.where(m, qd, zero), ki) for m in head_mask]
            full = dot_t0(ke, v)
            inc[way, c] = jnp.concatenate(
                [full[h * HEAD_K : (h + 1) * HEAD_K, h * HEAD_V : (h + 1) * HEAD_V] for h in range(heads)], axis=0
            )
            dec[way, c] = jnp.exp(dot_t0(jnp.concatenate([hi, lo], axis=0), ones))
        for h in range(heads):
            s = jnp.where(lower, scores[0][h], 0.0) + jnp.where(upper, scores[1][h], 0.0)
            out_acc[span, h * HEAD_V : (h + 1) * HEAD_V] = dot(s.astype(bf16), v[:, h * HEAD_V : (h + 1) * HEAD_V])
        return carry

    lax.fori_loop(0, chunks, first, 0)

    state_shape = (key_w, HEAD_V)
    for way in range(2):

        def total(i, carry):
            state, decay = carry
            c = i if way == 0 else chunks - 1 - i
            d = dec[way, c]
            return d * state + inc[way, c], d * decay

        state, decay = lax.fori_loop(0, chunks, total, (jnp.zeros(state_shape, f32), jnp.ones(state_shape, f32)))
        msg[way, 0:key_w, :] = state.astype(bf16)
        msg[way, key_w : 2 * key_w, :] = decay.astype(bf16)

    got[me_sp] = jnp.zeros(got.shape[1:], bf16)
    state_copies = []
    for o in range(1, sp):
        peer = lax.rem(me_sp + o, sp)
        way = jnp.where(peer > me_sp, 0, 1)
        copy = pltpu.make_async_remote_copy(
            src_ref=msg.at[way], dst_ref=got.at[me_sp],
            send_sem=st_send.at[o - 1], recv_sem=st_recv.at[o - 1],
            device_id=(peer, me_tp), device_id_type=MESH,
        )
        copy.start()
        state_copies.append(copy)
    if steps > 1:
        ring_start(2)
    for copy in state_copies:
        copy.wait()

    for way in range(2):

        def hop(i, state):
            at = i if way == 0 else sp - 1 - i
            reached = at < me_sp if way == 0 else at > me_sp
            block = got[at]
            new = block[key_w : 2 * key_w, :].astype(f32) * state + block[0:key_w, :].astype(f32)
            return jnp.where(reached, new, state)

        start = lax.fori_loop(0, sp, hop, jnp.zeros(state_shape, f32))

        def enter(i, state):
            c = i if way == 0 else chunks - 1 - i
            state_in[c, way * key_w : (way + 1) * key_w, :] = state.astype(bf16)
            return dec[way, c] * state + inc[way, c]

        lax.fori_loop(0, chunks, enter, start)

    def second(c, carry):
        span = pl.ds(pl.multiple_of(c * CHUNK, CHUNK), CHUNK)
        qf, qb = q_dec[0, span, :], q_dec[1, span, :]
        state = state_in[c]
        for h in range(heads):
            cols = slice(h * HEAD_V, (h + 1) * HEAD_V)
            m = head_mask[h]
            both = jnp.concatenate([jnp.where(m, qf, zero), jnp.where(m, qb, zero)], axis=1)
            att = out_acc[span, cols] + dot(both, state)
            inv = lax.rsqrt(jnp.mean(att * att, axis=-1, keepdims=True) + norm_eps)
            g = gate_ref[span, cols].astype(f32)
            silu = g / (1.0 + jnp.exp(-g))
            gbuf[span, cols] = (att * inv * gain_ref[0:1, cols] * silu).astype(bf16)
        return carry

    own_cols = pl.ds(pl.multiple_of(me_tp * val_w, val_w), val_w)
    gated_copies = []
    half = chunks // 2
    for part in range(2):
        lax.fori_loop(part * half, (part + 1) * half, second, 0)
        span = pl.ds(part * half * CHUNK, half * CHUNK)
        for o in range(1, tp):
            copy = pltpu.make_async_remote_copy(
                src_ref=gbuf.at[span, :], dst_ref=gated_all.at[span, own_cols],
                send_sem=gx_send.at[part, o - 1], recv_sem=gx_recv.at[part, o - 1],
                device_id=(me_sp, lax.rem(me_tp + o, tp)), device_id_type=MESH,
            )
            copy.start()
            gated_copies.append(copy)
    own_gated = pltpu.make_async_copy(gbuf, gated_all.at[:, own_cols], loc_sem.at[1])
    own_gated.start()
    for step in range(3, steps + 1):
        ring_start(step)
    for way in range(2):
        for step in range(steps):
            ring[step][way].wait_send()
        ring[steps - 1][way].wait_recv()
    own_down.wait()
    for copy in stream_copies + gated_copies:
        copy.wait()
    own_stream.wait()
    own_gated.wait()


def attention(queries, keys, values, out_gate, decay_logit, head_gain, stream, down_weight):
    sp, tp = lax.axis_size("sp"), lax.axis_size("tp")
    rows, key_w = queries.shape
    val_w = values.shape[1]
    chunks = rows // CHUNK
    own_rows, width = stream.shape
    vmem = pl.BlockSpec(memory_space=pltpu.VMEM)
    hbm = pl.BlockSpec(memory_space=pl.ANY)
    dma = pltpu.SemaphoreType.DMA
    return pl.pallas_call(
        functools.partial(attention_kernel, sp, tp),
        out_shape=(
            jax.ShapeDtypeStruct((own_rows * tp, width), bf16),
            jax.ShapeDtypeStruct((rows, val_w * tp), bf16),
            jax.ShapeDtypeStruct((down_weight.shape[0], down_weight.shape[1] * sp), bf16),
        ),
        in_specs=[vmem] * 8,
        out_specs=(hbm, hbm, hbm),
        scratch_shapes=[
            pltpu.VMEM((2, rows, key_w), bf16),
            pltpu.VMEM((rows, val_w), f32),
            pltpu.VMEM((2, chunks, key_w, HEAD_V), f32),
            pltpu.VMEM((2, chunks, key_w, HEAD_V), f32),
            pltpu.VMEM((chunks, 2 * key_w, HEAD_V), bf16),
            pltpu.VMEM((2, 2 * key_w, HEAD_V), bf16),
            pltpu.VMEM((sp, 2 * key_w, HEAD_V), bf16),
            pltpu.VMEM((rows, val_w), bf16),
            dma((sp - 1,)), dma((sp - 1,)), dma((tp - 1,)), dma((tp - 1,)),
            dma((2, tp - 1)), dma((2, tp - 1)),
            dma((2, sp // 2)), dma((2, sp // 2)), dma((3,)),
        ],
        cost_estimate=pl.CostEstimate(flops=40_000_000_000, bytes_accessed=50_000_000, transcendentals=0),
        compiler_params=pltpu.CompilerParams(collective_id=0, has_side_effects=True),
        name="attention",
    )(queries, keys, values, out_gate, decay_logit, head_gain.reshape(1, val_w), stream, down_weight)


def local(
    queries, keys, values, out_gate, decay_logit, head_gain, out_weight, stream, mlp_gain, up_weight, down_weight
):
    up_full = lax.all_gather(up_weight, "sp", axis=0, tiled=True)
    tp_index = lax.axis_index("tp")
    stream_all, gated_all, down_full = attention(
        queries, keys, values, out_gate, decay_logit, head_gain, stream, down_weight
    )
    own_rows = stream.shape[0]
    residual = (
        jnp.dot(gated_all, out_weight, preferred_element_type=f32) + stream_all.astype(f32)
    ).astype(bf16)
    wide = residual.astype(f32)
    normed = (wide * lax.rsqrt(jnp.mean(wide * wide, axis=-1, keepdims=True) + norm_eps) * mlp_gain).astype(bf16)
    hidden = jnp.square(jax.nn.relu(jnp.dot(normed, up_full, preferred_element_type=f32))).astype(bf16)
    mlp_sum = lax.psum_scatter(
        jnp.dot(hidden, down_full, preferred_element_type=f32).astype(bf16), "tp", scatter_dimension=0, tiled=True
    ).astype(f32)
    own = lax.dynamic_slice_in_dim(residual, tp_index * own_rows, own_rows, 0)
    return (own.astype(f32) + mlp_sum).astype(bf16)


def solution(mesh):
    in_specs = (
        P("sp", "tp"), P("sp", "tp"), P("sp", "tp"), P("sp", "tp"), P(None, "sp", "tp"), P("tp"), P(),
        P(("sp", "tp"), None), P(), P("sp", "tp"), P("tp", "sp"),
    )
    return jax.shard_map(local, mesh=mesh, in_specs=in_specs, out_specs=P(("sp", "tp"), None), check_vma=False)
```
